32 devices in a mesh: sp: 16 (over z, y, x), tp: 2 (over core).
Axes of the slice: x: 2, y: 2, z: 4, core: 2. Of those that a mesh axis runs over, the one named last changes fastest.
Arguments:
- queries: bfloat16 [4096, 512], P('sp', 'tp'), may hold values from -6 to 6
- keys: bfloat16 [4096, 512], P('sp', 'tp'), may hold values from -6 to 6
- values: bfloat16 [4096, 512], P('sp', 'tp'), may hold values from -6 to 6
- gains: float32 [2, 128], replicated, may hold values from 0.1 to 1.9
- bias_table: float32 [192, 4], P(None, 'tp'), may hold values from -6 to 270
- d_out: bfloat16 [4096, 512], P('sp', 'tp'), may hold values from -32 to 32
Outputs:
- d_queries: bfloat16 [4096, 512], P('sp', 'tp')
- d_keys: bfloat16 [4096, 512], P('sp', 'tp')
- d_values: bfloat16 [4096, 512], P('sp', 'tp')
- d_table: float32 [192, 4], P(None, 'tp')
- d_gains: float32 [2, 128], replicated
The draws below stay inside these ranges and needn't reach their ends.
All inputs are finite; a program needn't handle non-finite values.
Results may differ from the reference program's by a relative error of at most 0.008.
Values may be sent and summed in bfloat16 or wider, within the bound.
A program may use at most 64 MiB of HBM per device.

```python
import jax
import jax.numpy as jnp
from jax import lax

HEADS = 4
HEAD_DIM = 128
SEG = 64
LEFT = 4
MAX_REL = 128
TOKENS = 4096


def draw_bias_table(key, part):
    entries = MAX_REL + SEG
    rough = jnp.clip(jax.random.normal(key, (entries, HEADS), jnp.float32), -6.0, 6.0)
    return rough.astype(jnp.float32)


def draw_d_out(key, part):
    width = HEADS * HEAD_DIM
    position = jnp.arange(TOKENS).astype(jnp.float32)[:, None] / TOKENS
    spread = 10.0 ** (jax.random.uniform(jax.random.fold_in(key, 1), (TOKENS, 1), jnp.float32) - 1.0)
    base = jnp.clip(jax.random.normal(jax.random.fold_in(key, 2), (TOKENS, width), jnp.float32), -6.0, 6.0)
    rise = 3.0 ** position
    return (base * spread * rise).astype(jnp.bfloat16)


def shard_levels(own_key, dims, shards, smallest, high):
    gain = 1.0
    for axis_at, shards_of in shards:
        heights = jax.random.uniform(jax.random.fold_in(jax.random.fold_in(own_key, 6), axis_at), (shards_of,), jnp.float32, smallest / len(shards), high / len(shards))
        gain = gain * jnp.repeat(jnp.exp(heights), dims[axis_at] // shards_of).reshape((-1,) + (1,) * (len(dims) - 1 - axis_at))
    return gain


def centred(own_key, shape, scale, bound, cuts=(), held_as=jnp.bfloat16):
    values = scale * jax.random.normal(own_key, shape, jnp.float32)
    if cuts:
        values = values * shard_levels(own_key, shape, cuts, -0.22, 0.18)
    return jnp.clip(values, -bound, bound).astype(held_as)


def setup_inputs(seed: int = 0) -> dict:
    streams_of = jax.random.split(jax.random.key(seed), 7)
    return {
        "queries": centred(streams_of[0], (TOKENS, HEADS * HEAD_DIM), 1.0, 6.0, ((0, 16), (1, 2))),
        "keys": centred(streams_of[1], (TOKENS, HEADS * HEAD_DIM), 1.0, 6.0, ((0, 16), (1, 2))),
        "values": centred(streams_of[2], (TOKENS, HEADS * HEAD_DIM), 1.0, 6.0, ((0, 16), (1, 2))),
        "gains": jnp.clip(1.0 + 0.18 * jax.random.normal(streams_of[3], (2, HEAD_DIM), jnp.float32), 0.1, 1.9),
        "bias_table": draw_bias_table(jax.random.fold_in(streams_of[6], 71), 0),
        "d_out": draw_d_out(jax.random.fold_in(streams_of[6], 71), 0),
    }


EPSILON = 1e-06

def unit_rows(row_block):
    widened = row_block.astype(jnp.float32).reshape(row_block.shape[0], HEADS, HEAD_DIM)
    inv_rms = lax.rsqrt(lax.optimization_barrier(jnp.mean(widened * widened, axis=-1, keepdims=True)) + EPSILON)
    return (widened * inv_rms, inv_rms)

def rows_back(d_normed, row_block, gain_vec):
    unit_part, inv_rms = unit_rows(row_block)
    d_unit = d_normed * gain_vec
    d_rows = inv_rms * (d_unit - unit_part * lax.optimization_barrier(jnp.mean(d_unit * unit_part, axis=-1, keepdims=True)))
    return (d_rows.reshape(row_block.shape[0], -1).astype(jnp.bfloat16), lax.optimization_barrier(jnp.sum(d_normed * unit_part, axis=(0, 1))))

def lowered(array_in):
    return lax.optimization_barrier(array_in.astype(jnp.bfloat16)).astype(jnp.float32)

def reference(queries, keys, values, gains, bias_table, d_out):
    tail_rows = LEFT * SEG
    blocks = TOKENS // tail_rows
    factor = HEAD_DIM ** (-0.5)
    q_unit, _ = unit_rows(queries)
    q_norm = (q_unit * gains[0]).astype(jnp.bfloat16)
    k_unit, _ = unit_rows(keys)
    k_norm = (k_unit * gains[1]).astype(jnp.bfloat16)
    leading = jnp.zeros((tail_rows, HEADS, HEAD_DIM), jnp.bfloat16)
    k_all = jnp.concatenate([leading, k_norm])
    v_all = jnp.concatenate([leading, values.reshape(TOKENS, HEADS, HEAD_DIM)])
    q_blocks = q_norm.reshape(blocks, tail_rows, HEADS, HEAD_DIM)
    do_blocks = d_out.reshape(blocks, tail_rows, HEADS, HEAD_DIM)
    query_idx = jnp.arange(tail_rows, dtype=jnp.int32)[:, None]
    key_idx = jnp.arange(2 * tail_rows, dtype=jnp.int32)[None, :]
    rel_index = (jnp.clip(query_idx + tail_rows - key_idx, -(SEG - 1), MAX_REL) + SEG - 1).astype(jnp.int32)
    bias_tiles = jnp.transpose(bias_table[rel_index], (2, 0, 1))
    flat_index = rel_index.reshape(-1)

    def advance(state, entry):
        pend_k, pend_v, table_sum = state
        number, q_block, do_block = entry
        start = number * tail_rows
        k_ext = lax.dynamic_slice_in_dim(k_all, start, 2 * tail_rows, 0).astype(jnp.float32)
        v_ext = lax.dynamic_slice_in_dim(v_all, start, 2 * tail_rows, 0).astype(jnp.float32)
        query_seg = (start + query_idx) // SEG
        key_pos = start - tail_rows + key_idx
        key_seg = key_pos // SEG
        key_valid = (key_pos >= 0) & (key_seg >= query_seg - LEFT) & (key_seg <= query_seg)
        q_float = q_block.astype(jnp.float32)
        do_float = do_block.astype(jnp.float32)
        scores = jnp.einsum('ihd,jhd->hij', q_float, k_ext) * factor + bias_tiles
        scores = jnp.where(key_valid[None], scores, -jnp.inf)
        row_max = lax.optimization_barrier(jnp.max(scores, axis=-1, keepdims=True))
        log_total = row_max + jnp.log(lax.optimization_barrier(jnp.sum(jnp.exp(scores - row_max), axis=-1, keepdims=True)))
        prob = jnp.exp(scores - log_total)
        d_prob = jnp.einsum('ihd,jhd->hij', do_float, v_ext)
        row_delta = lax.optimization_barrier(jnp.sum(prob * d_prob, axis=-1, keepdims=True))
        d_score = prob * (d_prob - row_delta)
        prob_low = lowered(prob)
        d_low = lowered(d_score)
        grad_v = jnp.einsum('hij,ihd->jhd', prob_low, do_float)
        grad_k = jnp.einsum('hij,ihd->jhd', d_low, q_float) * factor
        grad_q = jnp.einsum('hij,jhd->ihd', d_low, k_ext) * factor
        table_part = jax.ops.segment_sum(jnp.transpose(d_score, (1, 2, 0)).reshape(-1, HEADS), flat_index, num_segments=MAX_REL + SEG)
        emitted = (pend_k + grad_k[:tail_rows], pend_v + grad_v[:tail_rows], grad_q)
        return ((grad_k[tail_rows:], grad_v[tail_rows:], table_sum + table_part), emitted)
    zero_rows = jnp.zeros((tail_rows, HEADS, HEAD_DIM), jnp.float32)
    initial = (zero_rows, zero_rows, jnp.zeros((MAX_REL + SEG, HEADS), jnp.float32))
    numbers = jnp.arange(blocks, dtype=jnp.int32)
    (last_k, last_v, d_table), (ys_k, ys_v, ys_q) = lax.scan(advance, initial, (numbers, q_blocks, do_blocks))
    d_kn = jnp.concatenate([ys_k[1:].reshape(-1, HEADS, HEAD_DIM), last_k])
    d_vn = jnp.concatenate([ys_v[1:].reshape(-1, HEADS, HEAD_DIM), last_v])
    d_qn = ys_q.reshape(TOKENS, HEADS, HEAD_DIM)
    d_queries, gain_q = rows_back(d_qn, queries, gains[0])
    d_keys, gain_k = rows_back(d_kn, keys, gains[1])
    d_values = d_vn.reshape(TOKENS, -1).astype(jnp.bfloat16)
    return (d_queries, d_keys, d_values, d_table, jnp.stack([gain_q, gain_k]))
```

```python
import functools

import jax
import jax.numpy as jnp
from jax import lax
from jax.experimental import pallas as pl
from jax.experimental.pallas import tpu as pltpu
from jax.sharding import PartitionSpec as P

HEAD_DIM = 128
SEG = 64
LEFT = 4
MAX_REL = 128
EPSILON = 1e-06
NEG = -1e30
MESH = pl.DeviceIdType.MESH
F32 = jnp.float32
BF16 = jnp.bfloat16


def dot(a, b, contract, precision=None):
    return lax.dot_general(
        a, b, ((contract[:1], contract[1:]), ((), ())), preferred_element_type=F32, precision=precision
    )


def unit_of(block):
    wide = block.astype(F32)
    rms = lax.rsqrt(jnp.mean(wide * wide, axis=-1, keepdims=True) + EPSILON)
    return wide * rms, rms


def kernel(
    n_sp, n_tp,
    q_ref, k_ref, v_ref, do_ref, g_ref, t_ref,
    dq_ref, dk_ref, dv_ref, dt_ref, dg_ref,
    k_raw, k_ext, v_ext, q_nxt, do_nxt, bias, bias_t, dk_acc, dv_acc,
    st_out, st_in, red_src, red,
    send_sem, recv_sem, red_send, red_recv,
):
    rows, width = q_ref.shape
    heads = width // HEAD_DIM
    half = rows // 2
    window = rows + half
    entries = t_ref.shape[0]
    factor = HEAD_DIM ** (-0.5)
    sp, tp = lax.axis_index("sp"), lax.axis_index("tp")
    total = n_sp * n_tp
    me = sp * n_tp + tp
    has_prev, has_next = sp > 0, sp < n_sp - 1

    def place(offset):
        other = lax.rem(me + offset, total)
        return lax.div(other, n_tp), lax.rem(other, n_tp)

    barrier = pltpu.get_barrier_semaphore()

    @pl.loop(1, total)
    def _(offset):
        pl.semaphore_signal(barrier, inc=1, device_id=place(offset), device_id_type=MESH)

    pl.semaphore_wait(barrier, total - 1)

    def part(ref, index):
        return ref.at[pl.ds(index * half, half)]

    def send(slot, src, dst, to):
        return pltpu.make_async_remote_copy(
            src_ref=src, dst_ref=dst, send_sem=send_sem.at[slot], recv_sem=recv_sem.at[slot],
            device_id=(to, tp), device_id_type=MESH,
        )

    nxt, prv = sp + 1, sp - 1
    forward = [
        send(0, part(k_ref, 1), part(k_raw, 1), nxt),
        send(1, part(v_ref, 1), part(v_ext, 1), nxt),
        send(2, part(k_ref, 0), part(k_raw, 0), nxt),
        send(3, part(v_ref, 0), part(v_ext, 0), nxt),
    ]
    back = [
        send(4, part(q_ref, 0), part(q_nxt, 0), prv),
        send(5, part(do_ref, 0), part(do_nxt, 0), prv),
        send(6, part(q_ref, 1), part(q_nxt, 1), prv),
        send(7, part(do_ref, 1), part(do_nxt, 1), prv),
    ]
    stats = [send(8 + i, st_out.at[i], st_in.at[i], prv) for i in range(2)]

    @pl.when(has_next)
    def _():
        for copy in forward:
            copy.start()

    @pl.when(has_prev)
    def _():
        for copy in back:
            copy.start()

    @pl.when(jnp.logical_not(has_prev))
    def _():
        k_ext[0:rows, :] = jnp.zeros((rows, width), BF16)
        v_ext[0:rows, :] = jnp.zeros((rows, width), BF16)

    head = [slice(h * HEAD_DIM, (h + 1) * HEAD_DIM) for h in range(heads)]
    g0, g1 = g_ref[0:1, :], g_ref[1:2, :]

    row = lax.broadcasted_iota(jnp.int32, (half, rows), 0)
    col = lax.broadcasted_iota(jnp.int32, (half, rows), 1)
    flip = (
        lax.broadcasted_iota(jnp.int32, (entries, rows), 0)
        + lax.broadcasted_iota(jnp.int32, (entries, rows), 1)
        == entries - 1
    ).astype(F32)
    base = dot(t_ref[...], flip, (0, 0), lax.Precision.HIGHEST)
    for h in range(heads):
        far = base[h : h + 1, 0:1]
        near = pltpu.roll(
            jnp.broadcast_to(base[h : h + 1, :], (half, rows)), 0, 1, stride=1, stride_axis=0
        )
        near = jnp.where(col <= row, far, near)
        near = jnp.where((col >= rows - SEG) & (row < SEG), NEG, near)
        first = jnp.where((col < SEG) & (row >= SEG), NEG, jnp.broadcast_to(far, (half, rows)))
        bias[h, :, 0:half] = first[:, 0:half]
        bias[h, :, half:] = near
        bias_t[h, 0:half, :] = first[:, 0:half].T
        bias_t[h, half:, :] = near[:, 0:half].T

    v_ext[rows:, :] = v_ref[...]
    for h in range(heads):
        k_ext[rows:, head[h]] = (unit_of(k_ref[:, head[h]])[0] * g1).astype(BF16)

    lane = lax.broadcasted_iota(jnp.int32, (half, HEAD_DIM), 1)
    window_col = lax.broadcasted_iota(jnp.int32, (1, window), 1)
    d_band = [None] * heads
    gain_q = jnp.zeros((1, HEAD_DIM), F32)
    gain_k = jnp.zeros((1, HEAD_DIM), F32)
    for pair in (1, 0):
        @pl.when(has_prev)
        def _():
            forward[2 * (1 - pair)].wait_recv()
            for h in range(heads):
                block = k_raw[pair * half : (pair + 1) * half, head[h]]
                k_ext[pair * half : (pair + 1) * half, head[h]] = (unit_of(block)[0] * g1).astype(BF16)
            forward[2 * (1 - pair) + 1].wait_recv()

        own = slice(pair * half, (pair + 1) * half)
        span = slice(pair * half, pair * half + window)
        before = rows - pair * half
        absent = jnp.where((window_col < before) & jnp.logical_not(has_prev), NEG, 0.0)
        table = jnp.zeros((half, HEAD_DIM), F32)
        for h in range(heads):
            unit, rms = unit_of(q_ref[own, head[h]])
            q_norm = (unit * g0).astype(BF16)
            d_o = do_ref[own, head[h]]
            k_win, v_win = k_ext[span, head[h]], v_ext[span, head[h]]
            scores = dot(q_norm, k_win, (1, 1)) * factor + bias[h] + absent
            top = jnp.max(scores, axis=-1, keepdims=True)
            e = jnp.exp(scores - top)
            denom = jnp.sum(e, axis=-1, keepdims=True)
            prob = e * (1.0 / denom)
            d_prob = dot(d_o, v_win, (1, 1))
            delta = jnp.sum(prob * d_prob, axis=-1, keepdims=True)
            d_score = prob * (d_prob - delta)
            table = jnp.where(lane == 2 * h, top + jnp.log(denom), table)
            table = jnp.where(lane == 2 * h + 1, delta, table)
            prob_low, d_low = prob.astype(BF16), d_score.astype(BF16)
            d_qn = dot(d_low, k_win, (1, 0)) * factor
            d_v = dot(prob_low[:, before:], d_o, (0, 0))
            d_k = dot(d_low[:, before:], q_norm, (0, 0))
            if pair == 1:
                dk_acc[:, head[h]] = d_k
                dv_acc[:, head[h]] = d_v
                d_band[h] = d_score
            else:
                dk_acc[0:half, head[h]] += d_k
                dv_acc[0:half, head[h]] += d_v
                d_band[h] = d_band[h] + d_score
            grad = d_qn * g0
            out = rms * (grad - unit * jnp.mean(grad * unit, axis=-1, keepdims=True))
            dq_ref[own, head[h]] = out.astype(BF16)
            gain_q += jnp.sum(d_qn * unit, axis=0, keepdims=True)
            gain_k += jnp.sum(d_qn * q_norm.astype(F32), axis=0, keepdims=True)
        st_out[pair] = table.T[0:8, :]

        @pl.when(has_prev)
        def _():
            stats[pair].start()

    lines = []
    for h in range(heads):
        near = d_band[h][:, half:]
        near_part = jnp.where(col > row, near, 0.0)
        far_sum = jnp.sum(d_band[h][:, 0:half] + (near - near_part)[:, 0:half], keepdims=True)
        step = half // 2
        while step:
            near_part = near_part[0:step] + pltpu.roll(near_part[step : 2 * step], rows - step, 1)
            step //= 2
        near_part = jnp.where(col[0:1] == 0, far_sum, near_part)
        lines += [near_part[:, 0:half], near_part[:, half:]]
    lines += [gain_q, gain_k]
    lines += [jnp.zeros((8 - len(lines), HEAD_DIM), F32)]
    packed = jnp.concatenate(lines, axis=0)
    red_src[...] = packed
    slot = tp * n_sp + sp
    red[slot] = packed

    @pl.loop(1, total)
    def _(offset):
        pltpu.make_async_remote_copy(
            src_ref=red_src, dst_ref=red.at[slot], send_sem=red_send, recv_sem=red_recv,
            device_id=place(offset), device_id_type=MESH,
        ).start()

    @pl.when(has_next)
    def _():
        for pair in (0, 1):
            own = slice(pair * half, rows)
            src = slice(pair * half, (pair + 1) * half)
            count = rows - pair * half
            back[2 * pair].wait_recv()
            back[2 * pair + 1].wait_recv()
            stats[pair].wait_recv()
            for h in range(heads):
                q_norm = (unit_of(q_nxt[src, head[h]])[0] * g0).astype(BF16)
                d_o = do_nxt[src, head[h]]
                k_own = k_ext[rows + pair * half : 2 * rows, head[h]]
                v_own = v_ext[rows + pair * half : 2 * rows, head[h]]
                scores = dot(k_own, q_norm, (1, 1)) * factor + bias_t[h, 0:count, :]
                prob = jnp.exp(scores - st_in[pair, 2 * h : 2 * h + 1, :])
                d_prob = dot(v_own, d_o, (1, 1))
                d_score = prob * (d_prob - st_in[pair, 2 * h + 1 : 2 * h + 2, :])
                dv_acc[own, head[h]] += dot(prob.astype(BF16), d_o, (1, 0))
                dk_acc[own, head[h]] += dot(d_score.astype(BF16), q_norm, (1, 0))

    dv_ref[...] = dv_acc[...].astype(BF16)
    for h in range(heads):
        unit, rms = unit_of(k_ref[:, head[h]])
        grad = dk_acc[:, head[h]] * factor * g1
        out = rms * (grad - unit * jnp.mean(grad * unit, axis=-1, keepdims=True))
        dk_ref[:, head[h]] = out.astype(BF16)

    peers = red.at[pl.ds(0, total - 1)]
    pltpu.make_async_copy(peers, peers, red_recv).wait()
    everyone = jnp.sum(red[...], axis=0)
    mine = jnp.sum(red[pl.ds(tp * n_sp, n_sp)], axis=0)
    band = jnp.concatenate(
        [
            jnp.concatenate([mine[2 * h : 2 * h + 1], mine[2 * h + 1 : 2 * h + 2]], axis=1)
            for h in range(heads)
        ],
        axis=0,
    )
    dt_ref[...] = dot(flip, band, (1, 1), lax.Precision.HIGHEST)
    dg_ref[0:1, :] = everyone[2 * heads : 2 * heads + 1]
    dg_ref[1:2, :] = everyone[2 * heads + 1 : 2 * heads + 2] / g1

    pltpu.make_async_copy(peers, peers, red_send).wait()

    @pl.when(has_next)
    def _():
        for copy in forward:
            copy.wait_send()

    @pl.when(has_prev)
    def _():
        for copy in back + stats:
            copy.wait_send()


def solution(mesh):
    n_sp, n_tp = mesh.shape["sp"], mesh.shape["tp"]

    def local(queries, keys, values, gains, bias_table, d_out):
        rows, width = queries.shape
        heads = width // HEAD_DIM
        assert rows == LEFT * SEG and 2 * heads + 2 <= 8
        total = n_sp * n_tp
        act = jax.ShapeDtypeStruct((rows, width), BF16)
        half = rows // 2
        vmem = pl.BlockSpec(memory_space=pltpu.VMEM)
        return pl.pallas_call(
            functools.partial(kernel, n_sp, n_tp),
            out_shape=(
                act, act, act,
                jax.ShapeDtypeStruct(bias_table.shape, F32),
                jax.ShapeDtypeStruct(gains.shape, F32),
            ),
            in_specs=[vmem] * 6,
            out_specs=(vmem,) * 5,
            scratch_shapes=[
                pltpu.VMEM((rows, width), BF16),
                pltpu.VMEM((2 * rows, width), BF16),
                pltpu.VMEM((2 * rows, width), BF16),
                pltpu.VMEM((rows, width), BF16),
                pltpu.VMEM((rows, width), BF16),
                pltpu.VMEM((heads, half, rows + half), F32),
                pltpu.VMEM((heads, rows, half), F32),
                pltpu.VMEM((rows, width), F32),
                pltpu.VMEM((rows, width), F32),
                pltpu.VMEM((2, 8, half), F32),
                pltpu.VMEM((2, 8, half), F32),
                pltpu.VMEM((8, HEAD_DIM), F32),
                pltpu.VMEM((total, 8, HEAD_DIM), F32),
                pltpu.SemaphoreType.DMA((10,)),
                pltpu.SemaphoreType.DMA((10,)),
                pltpu.SemaphoreType.DMA,
                pltpu.SemaphoreType.DMA,
            ],
            compiler_params=pltpu.CompilerParams(collective_id=0, has_side_effects=True),
        )(queries, keys, values, d_out, gains, bias_table)

    in_specs = (P("sp", "tp"), P("sp", "tp"), P("sp", "tp"), P(), P(None, "tp"), P("sp", "tp"))
    out_specs = (P("sp", "tp"), P("sp", "tp"), P("sp", "tp"), P(None, "tp"), P())
    return jax.shard_map(local, mesh=mesh, in_specs=in_specs, out_specs=out_specs, check_vma=False)
```

```python
import functools

import jax
import jax.numpy as jnp
from jax import lax
from jax.experimental import pallas as pl
from jax.experimental.pallas import tpu as pltpu
from jax.sharding import PartitionSpec as P

HEAD_DIM = 128
SEG = 64
LEFT = 4
MAX_REL = 128
EPSILON = 1e-06
NEG = -1e30
MESH = pl.DeviceIdType.MESH
F32 = jnp.float32
BF16 = jnp.bfloat16


def dot(a, b, contract, precision=None):
    return lax.dot_general(
        a, b, ((contract[:1], contract[1:]), ((), ())), preferred_element_type=F32, precision=precision
    )


def unit_of(block):
    wide = block.astype(F32)
    rms = lax.rsqrt(jnp.mean(wide * wide, axis=-1, keepdims=True) + EPSILON)
    return wide * rms, rms


def kernel(
    n_sp, n_tp,
    q_hbm, k_hbm, v_hbm, do_hbm, g_hbm, t_hbm,
    dq_ref, dk_ref, dv_ref, dt_ref, dg_ref,
    q_ref, k_ref, do_ref, g_ref, t_ref, k_raw, k_ext, v_ext, q_nxt, do_nxt, bias, bias_t, dk_acc, dv_acc,
    st_out, st_in, red_src, red,
    load_sem, send_sem, recv_sem, red_send, red_recv,
):
    rows, width = q_ref.shape
    heads = width // HEAD_DIM
    half = rows // 2
    window = rows + half
    entries = t_ref.shape[1]
    factor = HEAD_DIM ** (-0.5)
    sp, tp = lax.axis_index("sp"), lax.axis_index("tp")
    total = n_sp * n_tp
    has_prev, has_next = sp > 0, sp < n_sp - 1

    v_ref = v_ext.at[pl.ds(rows, rows)]
    loads = [
        pltpu.make_async_copy(src, dst, load_sem.at[i])
        for i, (src, dst) in enumerate(
            [(k_hbm, k_ref), (v_hbm, v_ref), (q_hbm, q_ref), (do_hbm, do_ref), (g_hbm, g_ref), (t_hbm, t_ref)]
        )
    ]
    for load in loads:
        load.start()

    def everyone_else(action):
        for other in range(n_tp - 1):
            action(sp, lax.rem(tp + 1 + other, n_tp))

        @pl.loop(1, n_sp)
        def _(offset):
            at = sp + offset
            at = jnp.where(at >= n_sp, at - n_sp, at)
            for other in range(n_tp):
                action(at, other)

    barrier = pltpu.get_barrier_semaphore()
    everyone_else(
        lambda at, core: pl.semaphore_signal(barrier, inc=1, device_id=(at, core), device_id_type=MESH)
    )
    pl.semaphore_wait(barrier, total - 1)
    for load in loads:
        load.wait()

    def part(ref, index):
        return ref.at[pl.ds(index * half, half)]

    def send(slot, src, dst, to):
        return pltpu.make_async_remote_copy(
            src_ref=src, dst_ref=dst, send_sem=send_sem.at[slot], recv_sem=recv_sem.at[slot],
            device_id=(to, tp), device_id_type=MESH,
        )

    nxt, prv = sp + 1, sp - 1
    forward = [
        send(0, part(k_ref, 1), part(k_raw, 1), nxt),
        send(1, part(v_ref, 1), part(v_ext, 1), nxt),
        send(2, part(k_ref, 0), part(k_raw, 0), nxt),
        send(3, part(v_ref, 0), part(v_ext, 0), nxt),
    ]
    back = [
        send(4, part(q_ref, 0), part(q_nxt, 0), prv),
        send(5, part(do_ref, 0), part(do_nxt, 0), prv),
        send(6, part(q_ref, 1), part(q_nxt, 1), prv),
        send(7, part(do_ref, 1), part(do_nxt, 1), prv),
    ]
    stats = [send(8 + i, st_out.at[i], st_in.at[i], prv) for i in range(2)]

    def advance(done, started, gate=has_next):
        if done:
            @pl.when(has_next)
            def _():
                for copy in done:
                    copy.wait_send()

        @pl.when(gate)
        def _():
            for copy in started:
                copy.start()

    advance([], forward[:2])

    @pl.when(jnp.logical_not(has_prev))
    def _():
        k_ext[0:rows, :] = jnp.zeros((rows, width), BF16)
        v_ext[0:rows, :] = jnp.zeros((rows, width), BF16)

    head = [slice(h * HEAD_DIM, (h + 1) * HEAD_DIM) for h in range(heads)]
    g0, g1 = g_ref[0:1, :], g_ref[1:2, :]

    row = lax.broadcasted_iota(jnp.int32, (half, rows), 0)
    col = lax.broadcasted_iota(jnp.int32, (half, rows), 1)
    flip = (
        lax.broadcasted_iota(jnp.int32, (entries, rows), 0)
        + lax.broadcasted_iota(jnp.int32, (entries, rows), 1)
        == entries - 1
    ).astype(F32)
    base = dot(t_ref[...], flip, (1, 0), lax.Precision.HIGHEST)
    for h in range(heads):
        far = base[h : h + 1, 0:1]
        near = pltpu.roll(
            jnp.broadcast_to(base[h : h + 1, :], (half, rows)), 0, 1, stride=1, stride_axis=0
        )
        near = jnp.where(col <= row, far, near)
        near = jnp.where((col >= rows - SEG) & (row < SEG), NEG, near)
        first = jnp.where((col < SEG) & (row >= SEG), NEG, jnp.broadcast_to(far, (half, rows)))
        bias[h, :, 0:half] = first[:, 0:half]
        bias[h, :, half:] = near
        bias_t[h, 0:half, :] = first[:, 0:half].T
        bias_t[h, half:, :] = near[:, 0:half].T

    for h in range(heads):
        k_ext[rows:, head[h]] = (unit_of(k_ref[:, head[h]])[0] * g1).astype(BF16)

    advance(forward[:2], forward[2:])
    lane = lax.broadcasted_iota(jnp.int32, (half, HEAD_DIM), 1)
    window_col = lax.broadcasted_iota(jnp.int32, (1, window), 1)
    d_band = [None] * heads
    gain_q = jnp.zeros((1, HEAD_DIM), F32)
    gain_k = jnp.zeros((1, HEAD_DIM), F32)
    for pair in (1, 0):
        @pl.when(has_prev)
        def _():
            forward[2 * (1 - pair)].wait_recv()
            for h in range(heads):
                block = k_raw[pair * half : (pair + 1) * half, head[h]]
                k_ext[pair * half : (pair + 1) * half, head[h]] = (unit_of(block)[0] * g1).astype(BF16)
            forward[2 * (1 - pair) + 1].wait_recv()

        if pair == 0:
            advance(forward[2:], back, has_prev)
        own = slice(pair * half, (pair + 1) * half)
        span = slice(pair * half, pair * half + window)
        before = rows - pair * half
        absent = jnp.where((window_col < before) & jnp.logical_not(has_prev), NEG, 0.0)
        table = jnp.zeros((half, HEAD_DIM), F32)
        for h in range(heads):
            unit, rms = unit_of(q_ref[own, head[h]])
            q_norm = (unit * g0).astype(BF16)
            d_o = do_ref[own, head[h]]
            k_win, v_win = k_ext[span, head[h]], v_ext[span, head[h]]
            scores = dot(q_norm, k_win, (1, 1)) * factor + bias[h] + absent
            top = jnp.max(scores, axis=-1, keepdims=True)
            e = jnp.exp(scores - top)
            denom = jnp.sum(e, axis=-1, keepdims=True)
            prob = e * (1.0 / denom)
            d_prob = dot(d_o, v_win, (1, 1))
            delta = jnp.sum(prob * d_prob, axis=-1, keepdims=True)
            d_score = prob * (d_prob - delta)
            table = jnp.where(lane == 2 * h, top + jnp.log(denom), table)
            table = jnp.where(lane == 2 * h + 1, delta, table)
            prob_low, d_low = prob.astype(BF16), d_score.astype(BF16)
            d_qn = dot(d_low, k_win, (1, 0)) * factor
            d_v = dot(prob_low[:, before:], d_o, (0, 0))
            d_k = dot(d_low[:, before:], q_norm, (0, 0))
            if pair == 1:
                dk_acc[:, head[h]] = d_k
                dv_acc[:, head[h]] = d_v
                d_band[h] = d_score
            else:
                dk_acc[0:half, head[h]] += d_k
                dv_acc[0:half, head[h]] += d_v
                d_band[h] = d_band[h] + d_score
            grad = d_qn * g0
            out = rms * (grad - unit * jnp.mean(grad * unit, axis=-1, keepdims=True))
            dq_ref[own, head[h]] = out.astype(BF16)
            gain_q += jnp.sum(d_qn * unit, axis=0, keepdims=True)
            gain_k += jnp.sum(d_qn * q_norm.astype(F32), axis=0, keepdims=True)
        st_out[pair] = table.T[0:8, :]

        @pl.when(has_prev)
        def _():
            stats[pair].start()

    lines = []
    for h in range(heads):
        near = d_band[h][:, half:]
        near_part = jnp.where(col > row, near, 0.0)
        far_sum = jnp.sum(d_band[h][:, 0:half] + (near - near_part)[:, 0:half], keepdims=True)
        step = half // 2
        while step:
            near_part = near_part[0:step] + pltpu.roll(near_part[step : 2 * step], rows - step, 1)
            step //= 2
        near_part = jnp.where(col[0:1] == 0, far_sum, near_part)
        lines += [near_part[:, 0:half], near_part[:, half:]]
    lines += [gain_q, gain_k]
    lines += [jnp.zeros((8 - len(lines), HEAD_DIM), F32)]
    packed = jnp.concatenate(lines, axis=0)
    red_src[...] = packed
    slot = tp * n_sp + sp
    red[slot] = packed

    everyone_else(
        lambda at, core: pltpu.make_async_remote_copy(
            src_ref=red_src, dst_ref=red.at[slot], send_sem=red_send, recv_sem=red_recv,
            device_id=(at, core), device_id_type=MESH,
        ).start()
    )

    @pl.when(has_next)
    def _():
        for pair in (0, 1):
            own = slice(pair * half, rows)
            src = slice(pair * half, (pair + 1) * half)
            count = rows - pair * half
            back[2 * pair].wait_recv()
            back[2 * pair + 1].wait_recv()
            stats[pair].wait_recv()
            for h in range(heads):
                q_norm = (unit_of(q_nxt[src, head[h]])[0] * g0).astype(BF16)
                d_o = do_nxt[src, head[h]]
                k_own = k_ext[rows + pair * half : 2 * rows, head[h]]
                v_own = v_ext[rows + pair * half : 2 * rows, head[h]]
                scores = dot(k_own, q_norm, (1, 1)) * factor + bias_t[h, 0:count, :]
                prob = jnp.exp(scores - st_in[pair, 2 * h : 2 * h + 1, :])
                d_prob = dot(v_own, d_o, (1, 1))
                d_score = prob * (d_prob - st_in[pair, 2 * h + 1 : 2 * h + 2, :])
                dv_acc[own, head[h]] += dot(prob.astype(BF16), d_o, (1, 0))
                dk_acc[own, head[h]] += dot(d_score.astype(BF16), q_norm, (1, 0))

    dv_ref[...] = dv_acc[...].astype(BF16)
    for h in range(heads):
        unit, rms = unit_of(k_ref[:, head[h]])
        grad = dk_acc[:, head[h]] * factor * g1
        out = rms * (grad - unit * jnp.mean(grad * unit, axis=-1, keepdims=True))
        dk_ref[:, head[h]] = out.astype(BF16)

    peers = red.at[pl.ds(0, total - 1)]
    pltpu.make_async_copy(peers, peers, red_recv).wait()
    everyone = jnp.sum(red[...], axis=0)
    mine = jnp.sum(red[pl.ds(tp * n_sp, n_sp)], axis=0)
    band = jnp.concatenate(
        [
            jnp.concatenate([mine[2 * h : 2 * h + 1], mine[2 * h + 1 : 2 * h + 2]], axis=1)
            for h in range(heads)
        ],
        axis=0,
    )
    dt_ref[...] = dot(band, flip, (1, 1), lax.Precision.HIGHEST)
    dg_ref[0:1, :] = everyone[2 * heads : 2 * heads + 1]
    dg_ref[1:2, :] = everyone[2 * heads + 1 : 2 * heads + 2] / g1

    pltpu.make_async_copy(peers, peers, red_send).wait()

    @pl.when(has_prev)
    def _():
        for copy in back + stats:
            copy.wait_send()


def emit(*refs):
    sem = refs[-1]
    count = len(refs) // 2
    copies = [pltpu.make_async_copy(refs[i], refs[count + i], sem.at[i]) for i in range(count)]
    for copy in copies:
        copy.start()
    for copy in copies:
        copy.wait()


def solution(mesh):
    n_sp, n_tp = mesh.shape["sp"], mesh.shape["tp"]

    def local(queries, keys, values, gains, bias_table, d_out):
        rows, width = queries.shape
        heads = width // HEAD_DIM
        assert rows == LEFT * SEG and 2 * heads + 2 <= 8
        total = n_sp * n_tp
        act = jax.ShapeDtypeStruct((rows, width), BF16)
        half = rows // 2
        vmem = pl.BlockSpec(memory_space=pltpu.VMEM)
        shapes = (
            act, act, act,
            jax.ShapeDtypeStruct(bias_table.shape[::-1], F32),
            jax.ShapeDtypeStruct(gains.shape, F32),
        )
        parts = pl.pallas_call(
            functools.partial(kernel, n_sp, n_tp),
            out_shape=shapes,
            in_specs=[pl.BlockSpec(memory_space=pltpu.HBM)] * 6,
            out_specs=(vmem,) * 5,
            scratch_shapes=[
                pltpu.VMEM((rows, width), BF16),
                pltpu.VMEM((rows, width), BF16),
                pltpu.VMEM((rows, width), BF16),
                pltpu.VMEM(gains.shape, F32),
                pltpu.VMEM(bias_table.shape[::-1], F32),
                pltpu.VMEM((rows, width), BF16),
                pltpu.VMEM((2 * rows, width), BF16),
                pltpu.VMEM((2 * rows, width), BF16),
                pltpu.VMEM((rows, width), BF16),
                pltpu.VMEM((rows, width), BF16),
                pltpu.VMEM((heads, half, rows + half), F32),
                pltpu.VMEM((heads, rows, half), F32),
                pltpu.VMEM((rows, width), F32),
                pltpu.VMEM((rows, width), F32),
                pltpu.VMEM((2, 8, half), F32),
                pltpu.VMEM((2, 8, half), F32),
                pltpu.VMEM((8, HEAD_DIM), F32),
                pltpu.VMEM((total, 8, HEAD_DIM), F32),
                pltpu.SemaphoreType.DMA((6,)),
                pltpu.SemaphoreType.DMA((10,)),
                pltpu.SemaphoreType.DMA((10,)),
                pltpu.SemaphoreType.DMA,
                pltpu.SemaphoreType.DMA,
            ],
            compiler_params=pltpu.CompilerParams(
                collective_id=0, has_side_effects=True, vmem_limit_bytes=16 * 1024 * 1024
            ),
        )(*(
            pltpu.with_memory_space_constraint(x, pltpu.HBM)
            for x in (queries, keys, values, d_out, gains, bias_table.T)
        ))
        d_q, d_k, d_v, d_table, d_gains = pl.pallas_call(
            emit,
            out_shape=shapes,
            in_specs=[vmem] * 5,
            out_specs=(pl.BlockSpec(memory_space=pltpu.HBM),) * 5,
            scratch_shapes=[pltpu.SemaphoreType.DMA((5,))],
            compiler_params=pltpu.CompilerParams(vmem_limit_bytes=8 * 1024 * 1024),
        )(*parts)
        return d_q, d_k, d_v, d_table.T, d_gains

    in_specs = (P("sp", "tp"), P("sp", "tp"), P("sp", "tp"), P(), P(None, "tp"), P("sp", "tp"))
    out_specs = (P("sp", "tp"), P("sp", "tp"), P("sp", "tp"), P(None, "tp"), P())
    return jax.shard_map(local, mesh=mesh, in_specs=in_specs, out_specs=out_specs, check_vma=False)
```

```python
import functools

import jax
import jax.numpy as jnp
from jax import lax
from jax.experimental import pallas as pl
from jax.experimental.pallas import tpu as pltpu
from jax.sharding import PartitionSpec as P

HEAD_DIM = 128
SEG = 64
LEFT = 4
MAX_REL = 128
EPSILON = 1e-06
NEG = -1e30
MESH = pl.DeviceIdType.MESH
F32 = jnp.float32
BF16 = jnp.bfloat16


def dot(a, b, contract, precision=None):
    return lax.dot_general(
        a, b, ((contract[:1], contract[1:]), ((), ())), preferred_element_type=F32, precision=precision
    )


def unit_of(block):
    wide = block.astype(F32)
    rms = lax.rsqrt(jnp.mean(wide * wide, axis=-1, keepdims=True) + EPSILON)
    return wide * rms, rms


def kernel(
    n_sp, n_tp,
    q_hbm, k_hbm, v_hbm, do_hbm, g_hbm, t_hbm,
    dq_ref, dk_ref, dv_ref, dt_ref, dg_ref,
    q_ref, k_ref, do_ref, g_ref, t_ref, k_raw, k_ext, v_ext, q_nxt, do_nxt, bias, bias_t, dk_acc, dv_acc,
    st_out, st_in, one_src, one, two_src, two,
    load_sem, send_sem, recv_sem, red_sem,
):
    rows, width = q_ref.shape
    heads = width // HEAD_DIM
    half = rows // 2
    window = rows + half
    entries = t_ref.shape[1]
    factor = HEAD_DIM ** (-0.5)
    sp, tp = lax.axis_index("sp"), lax.axis_index("tp")
    has_prev, has_next = sp > 0, sp < n_sp - 1

    v_ref = v_ext.at[pl.ds(rows, rows)]
    loads = [
        pltpu.make_async_copy(src, dst, load_sem.at[i])
        for i, (src, dst) in enumerate(
            [(k_hbm, k_ref), (v_hbm, v_ref), (q_hbm, q_ref), (do_hbm, do_ref), (g_hbm, g_ref), (t_hbm, t_ref)]
        )
    ]
    for load in loads:
        load.start()

    side, team = lax.rem(sp, 2), lax.div(sp, 2)
    teams = n_sp // 2

    def team_mates(action):
        for other in range(1, n_tp):
            action(sp, lax.rem(tp + other, n_tp))
        for other in range(n_tp):
            action(2 * team + 1 - side, lax.rem(tp + other, n_tp))

    def other_teams(action):
        @pl.loop(1, teams)
        def _(offset):
            at = team + offset
            at = jnp.where(at >= teams, at - teams, at)
            action(2 * at + side, tp)

    def greet(at, core):
        pl.semaphore_signal(barrier, inc=1, device_id=(at, core), device_id_type=MESH)

    barrier = pltpu.get_barrier_semaphore()
    greet(lax.rem(sp + 1, n_sp), tp)
    greet(lax.rem(sp + n_sp - 1, n_sp), tp)
    team_mates(greet)
    other_teams(greet)
    mates = 2 * n_tp - 1
    pl.semaphore_wait(barrier, 2 + mates + teams - 1)
    for load in loads:
        load.wait()

    def part(ref, index):
        return ref.at[pl.ds(index * half, half)]

    def send(slot, src, dst, to):
        return pltpu.make_async_remote_copy(
            src_ref=src, dst_ref=dst, send_sem=send_sem.at[slot], recv_sem=recv_sem.at[slot],
            device_id=(to, tp), device_id_type=MESH,
        )

    nxt, prv = sp + 1, sp - 1
    forward = [
        send(0, part(k_ref, 1), part(k_raw, 1), nxt),
        send(1, part(v_ref, 1), part(v_ext, 1), nxt),
        send(2, part(k_ref, 0), part(k_raw, 0), nxt),
        send(3, part(v_ref, 0), part(v_ext, 0), nxt),
    ]
    back = [
        send(4, part(q_ref, 0), part(q_nxt, 0), prv),
        send(5, part(do_ref, 0), part(do_nxt, 0), prv),
        send(6, part(q_ref, 1), part(q_nxt, 1), prv),
        send(7, part(do_ref, 1), part(do_nxt, 1), prv),
    ]
    stats = [send(8 + i, st_out.at[i], st_in.at[i], prv) for i in range(2)]

    def advance(done, started, gate=has_next):
        if done:
            @pl.when(has_next)
            def _():
                for copy in done:
                    copy.wait_send()

        @pl.when(gate)
        def _():
            for copy in started:
                copy.start()

    advance([], forward[:2])

    @pl.when(jnp.logical_not(has_prev))
    def _():
        k_ext[0:rows, :] = jnp.zeros((rows, width), BF16)
        v_ext[0:rows, :] = jnp.zeros((rows, width), BF16)

    head = [slice(h * HEAD_DIM, (h + 1) * HEAD_DIM) for h in range(heads)]
    g0, g1 = g_ref[0:1, :], g_ref[1:2, :]

    row = lax.broadcasted_iota(jnp.int32, (half, rows), 0)
    col = lax.broadcasted_iota(jnp.int32, (half, rows), 1)
    flip = (
        lax.broadcasted_iota(jnp.int32, (entries, rows), 0)
        + lax.broadcasted_iota(jnp.int32, (entries, rows), 1)
        == entries - 1
    ).astype(F32)
    base = dot(t_ref[...], flip, (1, 0), lax.Precision.HIGHEST)
    for h in range(heads):
        far = base[h : h + 1, 0:1]
        near = pltpu.roll(
            jnp.broadcast_to(base[h : h + 1, :], (half, rows)), 0, 1, stride=1, stride_axis=0
        )
        near = jnp.where(col <= row, far, near)
        near = jnp.where((col >= rows - SEG) & (row < SEG), NEG, near)
        first = jnp.where((col < SEG) & (row >= SEG), NEG, jnp.broadcast_to(far, (half, rows)))
        bias[h, :, 0:half] = first[:, 0:half]
        bias[h, :, half:] = near
        bias_t[h, 0:half, :] = first[:, 0:half].T
        bias_t[h, half:, :] = near[:, 0:half].T

    for h in range(heads):
        k_ext[rows:, head[h]] = (unit_of(k_ref[:, head[h]])[0] * g1).astype(BF16)

    advance(forward[:2], forward[2:])
    lane = lax.broadcasted_iota(jnp.int32, (half, HEAD_DIM), 1)
    window_col = lax.broadcasted_iota(jnp.int32, (1, window), 1)
    d_band = [None] * heads
    gain_q = jnp.zeros((1, HEAD_DIM), F32)
    gain_k = jnp.zeros((1, HEAD_DIM), F32)
    for pair in (1, 0):
        @pl.when(has_prev)
        def _():
            forward[2 * (1 - pair)].wait_recv()
            for h in range(heads):
                block = k_raw[pair * half : (pair + 1) * half, head[h]]
                k_ext[pair * half : (pair + 1) * half, head[h]] = (unit_of(block)[0] * g1).astype(BF16)
            forward[2 * (1 - pair) + 1].wait_recv()

        if pair == 0:
            advance(forward[2:], back[:2], has_prev)
        own = slice(pair * half, (pair + 1) * half)
        span = slice(pair * half, pair * half + window)
        before = rows - pair * half
        absent = jnp.where((window_col < before) & jnp.logical_not(has_prev), NEG, 0.0)
        table = jnp.zeros((half, HEAD_DIM), F32)
        for h in range(heads):
            unit, rms = unit_of(q_ref[own, head[h]])
            q_norm = (unit * g0).astype(BF16)
            d_o = do_ref[own, head[h]]
            k_win, v_win = k_ext[span, head[h]], v_ext[span, head[h]]
            scores = dot(q_norm, k_win, (1, 1)) * factor + bias[h] + absent
            top = jnp.max(scores, axis=-1, keepdims=True)
            e = jnp.exp(scores - top)
            denom = jnp.sum(e, axis=-1, keepdims=True)
            prob = e * (1.0 / denom)
            d_prob = dot(d_o, v_win, (1, 1))
            delta = jnp.sum(prob * d_prob, axis=-1, keepdims=True)
            d_score = prob * (d_prob - delta)
            table = jnp.where(lane == 2 * h, top + jnp.log(denom), table)
            table = jnp.where(lane == 2 * h + 1, delta, table)
            prob_low, d_low = prob.astype(BF16), d_score.astype(BF16)
            d_qn = dot(d_low, k_win, (1, 0)) * factor
            d_v = dot(prob_low[:, before:], d_o, (0, 0))
            d_k = dot(d_low[:, before:], q_norm, (0, 0))
            if pair == 1:
                dk_acc[:, head[h]] = d_k
                dv_acc[:, head[h]] = d_v
                d_band[h] = d_score
            else:
                dk_acc[0:half, head[h]] += d_k
                dv_acc[0:half, head[h]] += d_v
                d_band[h] = d_band[h] + d_score
            grad = d_qn * g0
            out = rms * (grad - unit * jnp.mean(grad * unit, axis=-1, keepdims=True))
            dq_ref[own, head[h]] = out.astype(BF16)
            gain_q += jnp.sum(d_qn * unit, axis=0, keepdims=True)
            gain_k += jnp.sum(d_qn * q_norm.astype(F32), axis=0, keepdims=True)
        st_out[pair] = table.T[0:8, :]

        @pl.when(has_prev)
        def _():
            stats[pair].start()

    lines = []
    for h in range(heads):
        near = d_band[h][:, half:]
        near_part = jnp.where(col > row, near, 0.0)
        far_sum = jnp.sum(d_band[h][:, 0:half] + (near - near_part)[:, 0:half], keepdims=True)
        step = half // 2
        while step:
            near_part = near_part[0:step] + pltpu.roll(near_part[step : 2 * step], rows - step, 1)
            step //= 2
        near_part = jnp.where(col[0:1] == 0, far_sum, near_part)
        lines += [near_part[:, 0:half], near_part[:, half:]]
    lines += [gain_q, gain_k]
    lines += [jnp.zeros((8 - len(lines), HEAD_DIM), F32)]
    packed = jnp.concatenate(lines, axis=0)
    one_src[...] = packed
    place = side * n_tp + tp
    one[place] = packed
    team_mates(
        lambda at, core: pltpu.make_async_remote_copy(
            src_ref=one_src, dst_ref=one.at[place], send_sem=red_sem.at[0], recv_sem=red_sem.at[1],
            device_id=(at, core), device_id_type=MESH,
        ).start()
    )
    advance([], back[2:], has_prev)
    near_peers = one.at[pl.ds(0, mates)]
    pltpu.make_async_copy(near_peers, near_peers, red_sem.at[1]).wait()
    whole = jnp.sum(one[...], axis=0)
    same = one[tp] + one[n_tp + tp]
    line = lax.broadcasted_iota(jnp.int32, whole.shape, 0)
    joined = jnp.where(line < 2 * heads, same, whole)
    two_src[...] = joined
    two[team] = joined
    other_teams(
        lambda at, core: pltpu.make_async_remote_copy(
            src_ref=two_src, dst_ref=two.at[team], send_sem=red_sem.at[2], recv_sem=red_sem.at[3],
            device_id=(at, core), device_id_type=MESH,
        ).start()
    )

    @pl.when(has_next)
    def _():
        for pair in (0, 1):
            own = slice(pair * half, rows)
            src = slice(pair * half, (pair + 1) * half)
            count = rows - pair * half
            back[2 * pair].wait_recv()
            back[2 * pair + 1].wait_recv()
            stats[pair].wait_recv()
            for h in range(heads):
                q_norm = (unit_of(q_nxt[src, head[h]])[0] * g0).astype(BF16)
                d_o = do_nxt[src, head[h]]
                k_own = k_ext[rows + pair * half : 2 * rows, head[h]]
                v_own = v_ext[rows + pair * half : 2 * rows, head[h]]
                scores = dot(k_own, q_norm, (1, 1)) * factor + bias_t[h, 0:count, :]
                prob = jnp.exp(scores - st_in[pair, 2 * h : 2 * h + 1, :])
                d_prob = dot(v_own, d_o, (1, 1))
                d_score = prob * (d_prob - st_in[pair, 2 * h + 1 : 2 * h + 2, :])
                dv_acc[own, head[h]] += dot(prob.astype(BF16), d_o, (1, 0))
                dk_acc[own, head[h]] += dot(d_score.astype(BF16), q_norm, (1, 0))

    dv_ref[...] = dv_acc[...].astype(BF16)
    for h in range(heads):
        unit, rms = unit_of(k_ref[:, head[h]])
        grad = dk_acc[:, head[h]] * factor * g1
        out = rms * (grad - unit * jnp.mean(grad * unit, axis=-1, keepdims=True))
        dk_ref[:, head[h]] = out.astype(BF16)

    far_peers = two.at[pl.ds(0, teams - 1)]
    pltpu.make_async_copy(far_peers, far_peers, red_sem.at[3]).wait()
    mine = jnp.sum(two[...], axis=0)
    band = jnp.concatenate(
        [
            jnp.concatenate([mine[2 * h : 2 * h + 1], mine[2 * h + 1 : 2 * h + 2]], axis=1)
            for h in range(heads)
        ],
        axis=0,
    )
    dt_ref[...] = dot(band, flip, (1, 1), lax.Precision.HIGHEST)
    dg_ref[0:1, :] = mine[2 * heads : 2 * heads + 1]
    dg_ref[1:2, :] = mine[2 * heads + 1 : 2 * heads + 2] / g1

    pltpu.make_async_copy(near_peers, near_peers, red_sem.at[0]).wait()
    pltpu.make_async_copy(far_peers, far_peers, red_sem.at[2]).wait()

    @pl.when(has_prev)
    def _():
        for copy in back + stats:
            copy.wait_send()


def emit(*refs):
    sem = refs[-1]
    count = len(refs) // 2
    copies = [pltpu.make_async_copy(refs[i], refs[count + i], sem.at[i]) for i in range(count)]
    for copy in copies:
        copy.start()
    for copy in copies:
        copy.wait()


def solution(mesh):
    n_sp, n_tp = mesh.shape["sp"], mesh.shape["tp"]

    def local(queries, keys, values, gains, bias_table, d_out):
        rows, width = queries.shape
        heads = width // HEAD_DIM
        assert n_sp % 2 == 0 and n_sp > 2 and rows == LEFT * SEG and 2 * heads + 2 <= 8
        act = jax.ShapeDtypeStruct((rows, width), BF16)
        half = rows // 2
        vmem = pl.BlockSpec(memory_space=pltpu.VMEM)
        shapes = (
            act, act, act,
            jax.ShapeDtypeStruct(bias_table.shape[::-1], F32),
            jax.ShapeDtypeStruct(gains.shape, F32),
        )
        parts = pl.pallas_call(
            functools.partial(kernel, n_sp, n_tp),
            out_shape=shapes,
            in_specs=[pl.BlockSpec(memory_space=pltpu.HBM)] * 6,
            out_specs=(vmem,) * 5,
            scratch_shapes=[
                pltpu.VMEM((rows, width), BF16),
                pltpu.VMEM((rows, width), BF16),
                pltpu.VMEM((rows, width), BF16),
                pltpu.VMEM(gains.shape, F32),
                pltpu.VMEM(bias_table.shape[::-1], F32),
                pltpu.VMEM((rows, width), BF16),
                pltpu.VMEM((2 * rows, width), BF16),
                pltpu.VMEM((2 * rows, width), BF16),
                pltpu.VMEM((rows, width), BF16),
                pltpu.VMEM((rows, width), BF16),
                pltpu.VMEM((heads, half, rows + half), F32),
                pltpu.VMEM((heads, rows, half), F32),
                pltpu.VMEM((rows, width), F32),
                pltpu.VMEM((rows, width), F32),
                pltpu.VMEM((2, 8, half), F32),
                pltpu.VMEM((2, 8, half), F32),
                pltpu.VMEM((8, HEAD_DIM), F32),
                pltpu.VMEM((2 * n_tp, 8, HEAD_DIM), F32),
                pltpu.VMEM((8, HEAD_DIM), F32),
                pltpu.VMEM((n_sp // 2, 8, HEAD_DIM), F32),
                pltpu.SemaphoreType.DMA((6,)),
                pltpu.SemaphoreType.DMA((10,)),
                pltpu.SemaphoreType.DMA((10,)),
                pltpu.SemaphoreType.DMA((4,)),
            ],
            compiler_params=pltpu.CompilerParams(
                collective_id=0, has_side_effects=True, vmem_limit_bytes=16 * 1024 * 1024
            ),
        )(*(
            pltpu.with_memory_space_constraint(x, pltpu.HBM)
            for x in (queries, keys, values, d_out, gains, bias_table.T)
        ))
        d_q, d_k, d_v, d_table, d_gains = pl.pallas_call(
            emit,
            out_shape=shapes,
            in_specs=[vmem] * 5,
            out_specs=(pl.BlockSpec(memory_space=pltpu.HBM),) * 5,
            scratch_shapes=[pltpu.SemaphoreType.DMA((5,))],
            compiler_params=pltpu.CompilerParams(vmem_limit_bytes=8 * 1024 * 1024),
        )(*parts)
        return d_q, d_k, d_v, d_table.T, d_gains

    in_specs = (P("sp", "tp"), P("sp", "tp"), P("sp", "tp"), P(), P(None, "tp"), P("sp", "tp"))
    out_specs = (P("sp", "tp"), P("sp", "tp"), P("sp", "tp"), P(None, "tp"), P())
    return jax.shard_map(local, mesh=mesh, in_specs=in_specs, out_specs=out_specs, check_vma=False)
```
